32 devices in a mesh: sp: 16 (over z, y, x), tp: 2 (over core).
Axes of the slice: x: 2, y: 2, z: 4, core: 2. Of those that a mesh axis runs over, the one named last changes fastest.
Arguments:
- stream_in: bfloat16 [4096, 2048], P('sp'), may hold values from -6 to 6
- norm_gain: float32 [2, 2048], replicated, may hold values from 0.1 to 1.9
- value_weight: bfloat16 [2, 2048, 2048], P(None, 'sp', 'tp'), may hold values from -0.125 to 0.125
- gate_weight: bfloat16 [2, 2048, 2048], P(None, 'sp', 'tp'), may hold values from -0.125 to 0.125
- conv_taps: float32 [2, 31, 2048], P(None, None, 'tp'), may hold values from -5 to 5
- channel_gain: float32 [2, 2048], P(None, 'tp'), may hold values from 0.1 to 1.9
- out_weight: bfloat16 [2, 2048, 2048], P(None, 'tp', 'sp'), may hold values from -0.125 to 0.125
Outputs:
- stream_out: bfloat16 [4096, 2048], P('sp')
The draws below stay inside these ranges and needn't reach their ends.
All inputs are finite; a program needn't handle non-finite values.
Results may differ from the reference program's by a relative error of at most 0.015.
Values may be sent and summed in bfloat16 or wider, within the bound.
A program may use at most 64 MiB of HBM per device.

```python
import jax
import jax.numpy as jnp
from jax import lax

D = 2048
KERNEL = 31
LAYERS = 2
TOKENS = 4096


def draw_conv_taps(key, part):
    first, second = jax.random.split(jax.random.fold_in(key, 17))
    base = jnp.clip(jax.random.normal(first, (LAYERS, KERNEL, D), jnp.float32), -6.0, 6.0)
    blocks = jnp.exp(jax.random.uniform(second, (LAYERS, 1, 8), jnp.float32, -1.4, 1.4))
    scales = jnp.repeat(blocks, D // 8, axis=2)
    return base * scales / jnp.sqrt(jnp.float32(KERNEL))


def block_levels(key, shape, shards, low, top_value):
    def one(axis_at, parts):
        steps = jax.random.uniform(jax.random.fold_in(jax.random.fold_in(key, 6), axis_at), (parts,), jnp.float32, low / len(shards), top_value / len(shards))
        return jnp.repeat(jnp.exp(steps), shape[axis_at] // parts).reshape((-1,) + (1,) * (len(shape) - axis_at - 1))

    level = one(*shards[0])
    for cut in shards[1:]:
        level = level * one(*cut)
    return level


def scatter_about(rng, shape, width, limit, cuts=(), held_as=jnp.bfloat16):
    array = width * jax.random.normal(rng, shape, jnp.float32)
    if cuts:
        array = array * block_levels(rng, shape, cuts, -0.22, 0.18)
    return jnp.clip(array, -limit, limit).astype(held_as)


def setup_inputs(seed: int = 0) -> dict:
    splits = jax.random.split(jax.random.key(seed), 8)
    return {
        "stream_in": scatter_about(splits[0], (TOKENS, D), 1.0, 6.0, ((0, 16),)),
        "norm_gain": jnp.clip(1.0 + 0.18 * jax.random.normal(splits[1], (LAYERS, D), jnp.float32), 0.1, 1.9),
        "value_weight": scatter_about(splits[2], (LAYERS, D, D), D ** -0.5, 0.125, ((1, 16), (2, 2))),
        "gate_weight": scatter_about(splits[3], (LAYERS, D, D), D ** -0.5, 0.125, ((1, 16), (2, 2))),
        "conv_taps": draw_conv_taps(jax.random.fold_in(splits[7], 71), 0),
        "channel_gain": jnp.clip(1.0 + 0.18 * jax.random.normal(splits[5], (LAYERS, D), jnp.float32), 0.1, 1.9),
        "out_weight": scatter_about(splits[6], (LAYERS, D, D), D ** -0.5, 0.125, ((1, 2), (2, 16))),
    }


epsilon = 1e-05

def reference(stream_in, norm_gain, value_weight, gate_weight, conv_taps, channel_gain, out_weight):
    stream = stream_in
    for layer in range(LAYERS):
        wide = stream.astype(jnp.float32)
        normed = (wide * lax.rsqrt(lax.optimization_barrier(jnp.mean(wide * wide, axis=1, keepdims=True)) + epsilon) * norm_gain[layer]).astype(jnp.bfloat16)
        value = jnp.dot(normed, value_weight[layer], preferred_element_type=jnp.float32)
        gate = jnp.dot(normed, gate_weight[layer], preferred_element_type=jnp.float32)
        gated = (value * jax.nn.sigmoid(gate)).astype(jnp.bfloat16)
        padded = jnp.concatenate([jnp.zeros((KERNEL - 1, D), jnp.bfloat16), gated], axis=0).astype(jnp.float32)
        filtered = jnp.zeros((TOKENS, D), jnp.float32)
        for tap in range(KERNEL):
            filtered = filtered + conv_taps[layer, tap] * padded[tap:tap + TOKENS]
        mean_value = lax.optimization_barrier(jnp.mean(filtered, axis=1, keepdims=True))
        variance = lax.optimization_barrier(jnp.mean(filtered * filtered, axis=1, keepdims=True)) - mean_value * mean_value
        activated = jax.nn.silu((filtered - mean_value) * lax.rsqrt(variance + epsilon) * channel_gain[layer]).astype(jnp.bfloat16)
        branch = jnp.dot(activated, out_weight[layer], preferred_element_type=jnp.float32)
        stream = (wide + branch).astype(jnp.bfloat16)
    return stream
```

```python
import functools

import jax
import jax.numpy as jnp
from jax import lax
from jax.experimental import pallas as pl
from jax.experimental.pallas import tpu as pltpu
from jax.sharding import PartitionSpec as P

epsilon = 1e-05
MESH = pl.DeviceIdType.MESH
F32 = jnp.float32
BF16 = jnp.bfloat16
PAD = 32


def kernel(n, layers, taps_n, stream_in, gain, vw, gw, taps, cgain, ow, out,
           wv, wg, wo, nrm, gat, hsend, hrecv, fil, ssend, srecv, act,
           dsend, drecv, xsend, xrecv, strm,
           loc_sem, wx_send, wx_recv, ring_send, ring_recv, msg_send, msg_recv):
    ring = n // 2
    s = lax.axis_index("sp")
    c = lax.axis_index("tp")
    o, i = s // 2, s % 2
    toks, width = stream_in.shape
    group = 2 * toks
    rows, cols = vw.shape[1], vw.shape[2]
    ch = cols // 2
    half = width // 2

    def place(outer):
        z, y = outer // 2, outer % 2
        return (1 - y) * z + y * (ring - 1 - z)

    def outer_at(pos):
        h = pos // (ring // 2)
        return 2 * ((1 - h) * pos + h * (ring - 1 - pos)) + h

    p = place(o)
    nxt = outer_at((p + 1) % ring) * 2 + i
    prv = outer_at((p + ring - 1) % ring) * 2 + i
    mate = o * 2 + 1 - i
    up = ((o + 1) % ring) * 2 + i
    down = ((o + ring - 1) % ring) * 2 + i
    x_dev, d_dev, xd_dev = (mate, c), (s, 1 - c), (mate, 1 - c)

    barrier = pltpu.get_barrier_semaphore()
    everyone = [x_dev, d_dev, xd_dev, (nxt, c), (prv, c), (up, c), (down, c)]
    for dev in everyone:
        pl.semaphore_signal(barrier, inc=1, device_id=dev, device_id_type=MESH)
    pl.semaphore_wait(barrier, len(everyone))

    def al(v, m):
        return pl.multiple_of(v, m)

    my_rows = pl.ds(al(s * rows, rows), rows)
    my_cols = pl.ds(al(i * ch, ch), ch)
    mate_cols = pl.ds(al((1 - i) * ch, ch), ch)

    def weight_views(l, kind):
        if kind == 0:
            return vw.at[l, :, my_cols], vw.at[l, :, mate_cols], wv.at[l, my_rows, :]
        if kind == 1:
            return gw.at[l, :, my_cols], gw.at[l, :, mate_cols], wg.at[l, my_rows, :]
        return ow.at[l, my_cols, :], ow.at[l, mate_cols, :], wo.at[l, :, my_rows]

    local, crossed = {}, {}

    def start_local(l, kind):
        src, _, dst = weight_views(l, kind)
        local[l, kind] = pltpu.make_async_copy(src, dst, loc_sem.at[l * 3 + kind])
        local[l, kind].start()

    def start_cross(l, kind):
        _, src, dst = weight_views(l, kind)
        crossed[l, kind] = pltpu.make_async_remote_copy(
            src, dst, wx_send.at[l * 3 + kind], wx_recv.at[l * 3 + kind],
            device_id=x_dev, device_id_type=MESH)
        crossed[l, kind].start()

    pending = {}

    def chunk(l, grp, d, q, pos):
        src = outer_at(pos)
        if grp == 0:
            w = wv if d == 0 else wg
            return w.at[l, pl.ds(al((src * 2 + q) * rows, rows), rows), :]
        quarter = ch // 4
        return wo.at[l, pl.ds((d * 2 + q) * quarter, quarter),
                     pl.ds(al(src * 2 * rows, 2 * rows), 2 * rows)]

    ready = set()

    def own_ready(l, kind):
        if (l, kind) not in ready:
            ready.add((l, kind))
            local[l, kind].wait()
            crossed[l, kind].wait()

    def pump(l, grp, t):
        if t == 0:
            for kind in ((0, 1) if grp == 0 else (2,)):
                own_ready(l, kind)
        for q in range(2):
            for d in range(2):
                k = (l * 2 + grp) * 2 + d
                if t > 0:
                    pending[k, q].wait()
                if t < ring - 1:
                    pos = (p + ring - t) % ring if d == 0 else (p + t) % ring
                    ref = chunk(l, grp, d, q, pos)
                    pending[k, q] = pltpu.make_async_remote_copy(
                        ref, ref, ring_send.at[k, q], ring_recv.at[k, q, t],
                        device_id=(nxt if d == 0 else prv, c), device_id_type=MESH)
                    pending[k, q].start()

    queue = [(0, 1, t) for t in range(ring)]
    for l in range(1, layers):
        queue += [(l, 0, t) for t in range(ring)] + [(l, 1, t) for t in range(ring)]
    done = []

    def pumps(count):
        for _ in range(count):
            if queue:
                item = queue.pop(0)
                pump(*item)
                done.append(item)

    def finish(l, grp):
        while (l, grp, ring - 1) not in done:
            pumps(1)

    def message(slot, src, dst, dev):
        m = pltpu.make_async_remote_copy(src, dst, msg_send.at[slot], msg_recv.at[slot],
                                         device_id=dev, device_id_type=MESH)
        m.start()
        return m

    for l in range(layers):
        for kind in range(3):
            start_local(l, kind)
    start_cross(0, 0)
    start_cross(0, 1)

    own_tok = al(i * toks, toks)
    mate_tok = al((1 - i) * toks, toks)
    own_half = pl.ds(al(c * half, half), half)
    mate_half = pl.ds(al((1 - c) * half, half), half)
    tile = 128 if toks % 128 == 0 else toks
    per_layer = 8

    for l in range(layers):
        base = l * per_layer
        source = stream_in if l == 0 else strm.at[l - 1]

        def norm_step(r, _):
            at = al(r * 64, 64)
            wide = source[pl.ds(at, 64), :].astype(F32)
            scale = lax.rsqrt(jnp.mean(wide * wide, axis=1, keepdims=True) + epsilon)
            nrm[l, pl.ds(al(own_tok + at, 64), 64), :] = (wide * scale * gain[l:l + 1, :]).astype(BF16)
            return 0

        lax.fori_loop(0, toks // 64, norm_step, 0)
        spot = nrm.at[l, pl.ds(own_tok, toks), own_half]
        got = nrm.at[l, pl.ds(mate_tok, toks), own_half]
        gather = message(base + 0, spot, spot, x_dev)
        if l == 0:
            start_cross(0, 2)
            for ll in range(1, layers):
                for kind in range(3):
                    start_cross(ll, kind)
            for t in range(ring - 2):
                pump(0, 0, t)
            gather.wait()
            relay = message(base + 1, got, got, d_dev)
            pump(0, 0, ring - 2)
            pumps(1)
            pump(0, 0, ring - 1)
            pumps(1)
        else:
            pumps(3)
            gather.wait()
            relay = message(base + 1, got, got, d_dev)
            finish(l, 0)
        relay.wait()

        def gate_step(r, _):
            at = al(r * tile, tile)
            x = nrm[l, pl.ds(at, tile), :]
            value = jnp.dot(x, wv[l], preferred_element_type=F32)
            gate = jnp.dot(x, wg[l], preferred_element_type=F32)
            gated = (value * jax.nn.sigmoid(gate)).astype(BF16)
            gat[pl.ds(al(PAD + at, 32), tile), :] = gated.astype(F32)
            return 0

        lax.fori_loop(0, group // tile, gate_step, 0)
        hsend[l] = gat[group:group + PAD, :].astype(BF16)
        halo = message(base + 2, hsend.at[l], hrecv.at[l], (up, c))
        pumps(1)
        halo.wait()
        first = (o > 0).astype(F32)
        gat[0:PAD, :] = hrecv[l].astype(F32) * first

        lead = PAD - (taps_n - 1)
        step_rows = 64
        lanes = 128

        def conv_step(r, _):
            at = al(r * step_rows, step_rows)
            for lane in range(ch // lanes):
                cut = slice(lane * lanes, (lane + 1) * lanes)
                total = jnp.zeros((step_rows, lanes), F32)
                block = gat[pl.ds(at, step_rows + PAD), cut]
                for b in range(8):
                    moved = block if b == 0 else pltpu.roll(block, step_rows + PAD - b, 0)
                    for a in range(PAD // 8 + 1):
                        tap = 8 * a + b - lead
                        if 0 <= tap < taps_n:
                            total = total + taps[l, tap:tap + 1, cut] * moved[8 * a:8 * a + step_rows]
                fil[pl.ds(at, step_rows), cut] = total
            return 0

        parts = 2
        per = group // step_rows // parts
        for part in range(parts):
            lax.fori_loop(part * per, (part + 1) * per, conv_step, 0)
            pumps(1)

        wide = fil[...]
        first_sum = jnp.sum(wide, axis=1, keepdims=True)
        second_sum = jnp.sum(wide * wide, axis=1, keepdims=True)
        lane_id = lax.broadcasted_iota(jnp.int32, (group, lanes), 1)
        stat = jnp.where(lane_id == 0, first_sum, jnp.where(lane_id == 1, second_sum, 0.0))
        ssend[l] = jnp.transpose(stat)[0:8, :]
        sums = [message(base + 3 + k, ssend.at[l], srecv.at[l, k], dev)
                for k, dev in enumerate((x_dev, d_dev, xd_dev))]
        pumps(1)
        for m in sums:
            m.wait()
        whole = ssend[l] + srecv[l, 0] + srecv[l, 1] + srecv[l, 2]
        stat = jnp.transpose(jnp.concatenate([whole] + [jnp.zeros((lanes - 8, group), F32)], axis=0))
        mean_value = stat[:, 0:1] / width
        variance = stat[:, 1:2] / width - mean_value * mean_value
        act[...] = jax.nn.silu((fil[...] - mean_value) * lax.rsqrt(variance + epsilon)
                               * cgain[l:l + 1, pl.ds(al(i * ch, ch), ch)]).astype(BF16)
        finish(l, 1)

        def other_step(r, _):
            at = al(r * tile, tile)
            dsend[l, pl.ds(at, tile), :] = jnp.dot(
                act[pl.ds(at, tile), :], wo[l, :, mate_half], preferred_element_type=F32).astype(BF16)
            return 0

        lax.fori_loop(0, group // tile, other_step, 0)
        swap = message(base + 6, dsend.at[l], drecv.at[l], d_dev)
        swap.wait()

        def mate_step(r, _):
            at = al(mate_tok + r * tile, tile)
            mine = jnp.dot(act[pl.ds(at, tile), :], wo[l, :, own_half], preferred_element_type=F32)
            xsend[l, pl.ds(al(r * tile, tile), tile), :] = (
                mine + drecv[l, pl.ds(at, tile), :].astype(F32)).astype(BF16)
            return 0

        lax.fori_loop(0, toks // tile, mate_step, 0)
        scatter = message(base + 7, xsend.at[l], xrecv.at[l], x_dev)
        pumps(2)
        scatter.wait()

        def own_step(r, _):
            at = al(own_tok + r * tile, tile)
            here = pl.ds(al(r * tile, tile), tile)
            mine = jnp.dot(act[pl.ds(at, tile), :], wo[l, :, own_half], preferred_element_type=F32)
            branch = mine + drecv[l, pl.ds(at, tile), :].astype(F32) + xrecv[l, here, :].astype(F32)
            strm[l, here, own_half] = (source[here, own_half].astype(F32) + branch).astype(BF16)
            return 0

        lax.fori_loop(0, toks // tile, own_step, 0)
        piece = strm.at[l, :, own_half]
        message(layers * per_layer + l, piece, piece, d_dev).wait()

    out[...] = strm[layers - 1]


def fused(n, layers):
    def body(stream_in, norm_gain, value_weight, gate_weight, conv_taps, channel_gain, out_weight):
        toks, width = stream_in.shape
        taps_n = conv_taps.shape[1]
        rows, cols = value_weight.shape[1], value_weight.shape[2]
        ch, half, group, ring = cols // 2, width // 2, 2 * toks, n // 2
        i = lax.axis_index("sp") % 2
        taps = lax.dynamic_slice_in_dim(conv_taps, i * ch, ch, axis=2)
        vmem = pl.BlockSpec(memory_space=pltpu.VMEM)
        hbm = pl.BlockSpec(memory_space=pltpu.HBM)
        msgs = layers * 9
        return pl.pallas_call(
            functools.partial(kernel, n, layers, taps_n),
            out_shape=jax.ShapeDtypeStruct((toks, width), BF16),
            in_specs=[vmem, vmem, hbm, hbm, vmem, vmem, hbm],
            out_specs=vmem,
            scratch_shapes=[
                pltpu.VMEM((layers, width, ch), BF16),
                pltpu.VMEM((layers, width, ch), BF16),
                pltpu.VMEM((layers, ch, width), BF16),
                pltpu.VMEM((layers, group, width), BF16),
                pltpu.VMEM((PAD + group, ch), F32),
                pltpu.VMEM((layers, PAD, ch), BF16),
                pltpu.VMEM((layers, PAD, ch), BF16),
                pltpu.VMEM((group, ch), F32),
                pltpu.VMEM((layers, 8, group), F32),
                pltpu.VMEM((layers, 3, 8, group), F32),
                pltpu.VMEM((group, ch), BF16),
                pltpu.VMEM((layers, group, half), BF16),
                pltpu.VMEM((layers, group, half), BF16),
                pltpu.VMEM((layers, toks, half), BF16),
                pltpu.VMEM((layers, toks, half), BF16),
                pltpu.VMEM((layers, toks, width), BF16),
                pltpu.SemaphoreType.DMA((layers * 3,)),
                pltpu.SemaphoreType.DMA((layers * 3,)),
                pltpu.SemaphoreType.DMA((layers * 3,)),
                pltpu.SemaphoreType.DMA((layers * 4, 2)),
                pltpu.SemaphoreType.DMA((layers * 4, 2, ring - 1)),
                pltpu.SemaphoreType.DMA((msgs,)),
                pltpu.SemaphoreType.DMA((msgs,)),
            ],
            compiler_params=pltpu.CompilerParams(
                collective_id=0, has_side_effects=True, vmem_limit_bytes=62 * 2**20),
        )(stream_in, norm_gain, value_weight, gate_weight, taps, channel_gain, out_weight)

    return body


def passed_along(value, axis, steps):
    count = lax.axis_size(axis)
    leading, last = (max(0, -steps), min(count, count - steps))
    return lax.ppermute(value, axis, [(source, source + steps) for source in range(leading, last)])


def general(stream_in, norm_gain, value_weight, gate_weight, conv_taps, channel_gain, out_weight):
    stream = stream_in
    tok_rows = stream_in.shape[0]
    width = stream_in.shape[1]
    taps_n = conv_taps.shape[1]
    local_cols = value_weight.shape[2]
    for layer in range(norm_gain.shape[0]):
        wide = stream.astype(F32)
        normed = (
            wide
            * lax.rsqrt(jnp.mean(wide * wide, axis=1, keepdims=True) + epsilon)
            * norm_gain[layer]
        ).astype(BF16)
        value = jnp.dot(normed, lax.all_gather(value_weight[layer], "sp", axis=0, tiled=True),
                        preferred_element_type=F32)
        gate = jnp.dot(normed, lax.all_gather(gate_weight[layer], "sp", axis=0, tiled=True),
                       preferred_element_type=F32)
        gated = (value * jax.nn.sigmoid(gate)).astype(BF16)
        earlier = passed_along(gated[tok_rows - (taps_n - 1):], "sp", 1)
        padded = jnp.concatenate([earlier, gated], axis=0).astype(F32)
        taps = conv_taps[layer]
        filtered = jnp.zeros((tok_rows, local_cols), F32)
        for tap in range(taps_n):
            filtered = filtered + taps[tap] * padded[tap:tap + tok_rows]
        sum_first, sum_second = lax.psum(
            (jnp.sum(filtered, axis=1), jnp.sum(filtered * filtered, axis=1)), "tp")
        mean_value = (sum_first / width)[:, None]
        variance = (sum_second / width)[:, None] - mean_value * mean_value
        activated = jax.nn.silu(
            (filtered - mean_value) * lax.rsqrt(variance + epsilon) * channel_gain[layer]
        ).astype(BF16)
        whole_out = lax.all_gather(out_weight[layer], "sp", axis=1, tiled=True)
        terms = jnp.dot(activated, whole_out, preferred_element_type=F32)
        summed = lax.psum(terms.astype(BF16), "tp").astype(F32)
        stream = (wide + summed).astype(BF16)
    return stream


def solution(mesh):
    n, tp = mesh.shape["sp"], mesh.shape["tp"]

    def body(stream_in, norm_gain, value_weight, *rest):
        rows, cols = value_weight.shape[1], value_weight.shape[2]
        pairs = tp == 2 and n % 4 == 0 and rows % 128 == 0 and cols % 1024 == 0
        fits = stream_in.shape[0] % 64 == 0 and rest[1].shape[1] <= PAD
        chosen = fused(n, norm_gain.shape[0]) if pairs and fits else general
        return chosen(stream_in, norm_gain, value_weight, *rest)

    return jax.shard_map(
        body,
        mesh=mesh,
        in_specs=(
            P("sp", None),
            P(),
            P(None, "sp", "tp"),
            P(None, "sp", "tp"),
            P(None, None, "tp"),
            P(None, "tp"),
            P(None, "tp", "sp"),
        ),
        out_specs=P("sp", None),
        check_vma=False,
    )
```

```python
import functools

import jax
import jax.numpy as jnp
from jax import lax
from jax.experimental import pallas as pl
from jax.experimental.pallas import tpu as pltpu
from jax.sharding import PartitionSpec as P

epsilon = 1e-05
MESH = pl.DeviceIdType.MESH
F32 = jnp.float32
BF16 = jnp.bfloat16
PAD = 32
EARLY = 3
SPLIT = 1


def kernel(n, layers, taps_n, stream_in, gain, vw, gw, taps, cgain, ow, out,
           wv, wg, wo, nrm, gat, hsend, hrecv, fil, ssend, srecv, act,
           dsend, drecv, xsend, xrecv, strm, keep,
           loc_sem, wx_send, wx_recv, ring_send, ring_recv, msg_send, msg_recv):
    ring = n // 2
    s = lax.axis_index("sp")
    c = lax.axis_index("tp")
    o, i = s // 2, s % 2
    toks, width = stream_in.shape
    group = 2 * toks
    rows, cols = vw.shape[1], vw.shape[2]
    ch = cols // 2
    half = width // 2

    def place(outer):
        z, y = outer // 2, outer % 2
        return (1 - y) * z + y * (ring - 1 - z)

    def outer_at(pos):
        h = pos // (ring // 2)
        return 2 * ((1 - h) * pos + h * (ring - 1 - pos)) + h

    p = place(o)
    nxt = outer_at((p + 1) % ring) * 2 + i
    prv = outer_at((p + ring - 1) % ring) * 2 + i
    mate = o * 2 + 1 - i
    up = ((o + 1) % ring) * 2 + i
    down = ((o + ring - 1) % ring) * 2 + i
    x_dev, d_dev, xd_dev = (mate, c), (s, 1 - c), (mate, 1 - c)

    barrier = pltpu.get_barrier_semaphore()
    everyone = [x_dev, d_dev, xd_dev, (nxt, c), (prv, c), (up, c), (down, c)]
    for dev in everyone:
        pl.semaphore_signal(barrier, inc=1, device_id=dev, device_id_type=MESH)
    pl.semaphore_wait(barrier, len(everyone))

    def al(v, m):
        return pl.multiple_of(v, m)

    my_rows = pl.ds(al(s * rows, rows), rows)
    my_cols = pl.ds(al(i * ch, ch), ch)
    mate_cols = pl.ds(al((1 - i) * ch, ch), ch)

    def weight_views(l, kind):
        if kind == 0:
            return vw.at[l, :, my_cols], vw.at[l, :, mate_cols], wv.at[l, my_rows, :]
        if kind == 1:
            return gw.at[l, :, my_cols], gw.at[l, :, mate_cols], wg.at[l, my_rows, :]
        return ow.at[l, my_cols, :], ow.at[l, mate_cols, :], wo.at[l, :, my_rows]

    local, crossed = {}, {}

    def start_local(l, kind):
        src, _, dst = weight_views(l, kind)
        local[l, kind] = pltpu.make_async_copy(src, dst, loc_sem.at[l * 3 + kind])
        local[l, kind].start()

    def start_cross(l, kind):
        _, src, dst = weight_views(l, kind)
        crossed[l, kind] = pltpu.make_async_remote_copy(
            src, dst, wx_send.at[l * 3 + kind], wx_recv.at[l * 3 + kind],
            device_id=x_dev, device_id_type=MESH)
        crossed[l, kind].start()

    pending = {}

    def block_cols(pos, d):
        return pl.ds(al((outer_at(pos) * 2 + d) * rows, rows), rows)

    def chunk(l, grp, d, q, pos):
        if grp == 0:
            block = outer_at(pos) * 2 + (i + q // SPLIT) % 2
            w, size = (wv if d == 0 else wg), rows // SPLIT
            return w.at[l, pl.ds(al(block * rows + q % SPLIT * size, size), size), :]
        size = ch // 2 // SPLIT
        return wo.at[l, pl.ds(q * size, size), block_cols(pos, d)]

    def own_ready(l, grp, q):
        if grp == 0 and q % SPLIT == 0:
            for kind in (0, 1):
                (crossed if q else local)[l, kind].wait()
        if grp == 1 and q == 0:
            local[l, 2].wait()
            crossed[l, 2].wait()

    def pump(l, grp, t):
        for q in range(2 * SPLIT):
            if t == 0:
                own_ready(l, grp, q)
            for d in range(2):
                k = (l * 2 + grp) * 2 + d
                if t > 0:
                    pending[k, q].wait()
                if t < ring - 1:
                    pos = (p + ring - t) % ring if d == 0 else (p + t) % ring
                    ref = chunk(l, grp, d, q, pos)
                    pending[k, q] = pltpu.make_async_remote_copy(
                        ref, ref, ring_send.at[k, q], ring_recv.at[k, q, t],
                        device_id=(nxt if d == 0 else prv, c), device_id_type=MESH)
                    pending[k, q].start()

    queue = []
    for l in range(layers):
        main = [(l, 0, t) for t in range(1 if l else 0, ring)]
        side = [(l, 1, t) for t in range(ring)]
        early = min(EARLY, ring)
        queue += main[:len(main) - early]
        for t in range(early):
            queue += [main[len(main) - early + t], side[t]]
        rest = side[early:]
        queue += rest[:len(rest) // 2]
        if l + 1 < layers:
            queue.append((l + 1, 0, 0))
        queue += rest[len(rest) // 2:]
    done = []

    def pumps(count):
        for _ in range(count):
            if queue:
                item = queue.pop(0)
                pump(*item)
                done.append(item)

    def ensure(l, grp, t):
        while (l, grp, t) not in done:
            pumps(1)

    def message(slot, src, dst, dev):
        m = pltpu.make_async_remote_copy(src, dst, msg_send.at[slot], msg_recv.at[slot],
                                         device_id=dev, device_id_type=MESH)
        m.start()
        return m

    for l in range(layers):
        for kind in range(3):
            start_local(l, kind)
    start_cross(0, 0)
    start_cross(0, 1)

    own_tok = al(i * toks, toks)
    mate_tok = al((1 - i) * toks, toks)
    own_half = pl.ds(al(c * half, half), half)
    tile = 128 if toks % 128 == 0 else toks
    per_layer = 6 + ring * 3

    for l in range(layers):
        base = l * per_layer
        source = stream_in if l == 0 else strm.at[l - 1]

        def norm_step(r, _):
            at = al(r * 64, 64)
            wide = source[pl.ds(at, 64), :].astype(F32)
            scale = lax.rsqrt(jnp.mean(wide * wide, axis=1, keepdims=True) + epsilon)
            nrm[l, pl.ds(al(own_tok + at, 64), 64), :] = (wide * scale * gain[l:l + 1, :]).astype(BF16)
            return 0

        lax.fori_loop(0, toks // 64, norm_step, 0)
        spot = nrm.at[l, pl.ds(own_tok, toks), own_half]
        got = nrm.at[l, pl.ds(mate_tok, toks), own_half]
        gather = message(base + 0, spot, spot, x_dev)
        if l == 0:
            start_cross(0, 2)
            for ll in range(1, layers):
                for kind in range(3):
                    start_cross(ll, kind)
            pumps(3)
        else:
            pumps(2)
        gather.wait()
        relay = message(base + 1, got, got, d_dev)
        ensure(l, 0, ring - 1)
        relay.wait()

        def gate_step(r, _):
            at = al(r * tile, tile)
            x = nrm[l, pl.ds(at, tile), :]
            value = jnp.dot(x, wv[l], preferred_element_type=F32)
            gate = jnp.dot(x, wg[l], preferred_element_type=F32)
            gated = (value * jax.nn.sigmoid(gate)).astype(BF16)
            gat[pl.ds(al(PAD + at, 32), tile), :] = gated.astype(F32)
            return 0

        lax.fori_loop(0, group // tile, gate_step, 0)
        hsend[l] = gat[group:group + PAD, :].astype(BF16)
        halo = message(base + 2, hsend.at[l], hrecv.at[l], (up, c))
        pumps(1)
        halo.wait()
        first = (o > 0).astype(F32)
        gat[0:PAD, :] = hrecv[l].astype(F32) * first

        lead = PAD - (taps_n - 1)
        step_rows = 64
        lanes = 128

        def conv_step(r, _):
            at = al(r * step_rows, step_rows)
            for lane in range(ch // lanes):
                cut = slice(lane * lanes, (lane + 1) * lanes)
                total = jnp.zeros((step_rows, lanes), F32)
                block = gat[pl.ds(at, step_rows + PAD), cut]
                for b in range(8):
                    moved = block if b == 0 else pltpu.roll(block, step_rows + PAD - b, 0)
                    for a in range(PAD // 8 + 1):
                        tap = 8 * a + b - lead
                        if 0 <= tap < taps_n:
                            total = total + taps[l, tap:tap + 1, cut] * moved[8 * a:8 * a + step_rows]
                fil[pl.ds(at, step_rows), cut] = total
            return 0

        parts = 2
        per = group // step_rows // parts
        for part in range(parts):
            lax.fori_loop(part * per, (part + 1) * per, conv_step, 0)
            pumps(1)

        wide = fil[...]
        first_sum = jnp.sum(wide, axis=1, keepdims=True)
        second_sum = jnp.sum(wide * wide, axis=1, keepdims=True)
        lane_id = lax.broadcasted_iota(jnp.int32, (group, lanes), 1)
        stat = jnp.where(lane_id == 0, first_sum, jnp.where(lane_id == 1, second_sum, 0.0))
        ssend[l] = jnp.transpose(stat)[0:8, :]
        sums = [message(base + 3 + k, ssend.at[l], srecv.at[l, k], dev)
                for k, dev in enumerate((x_dev, d_dev, xd_dev))]
        pumps(1)
        for m in sums:
            m.wait()
        whole = ssend[l] + srecv[l, 0] + srecv[l, 1] + srecv[l, 2]
        stat = jnp.transpose(jnp.concatenate([whole] + [jnp.zeros((lanes - 8, group), F32)], axis=0))
        mean_value = stat[:, 0:1] / width
        variance = stat[:, 1:2] / width - mean_value * mean_value
        act[...] = jax.nn.silu((fil[...] - mean_value) * lax.rsqrt(variance + epsilon)
                               * cgain[l:l + 1, pl.ds(al(i * ch, ch), ch)]).astype(BF16)

        slot = base + 6
        own_rows, mate_rows = pl.ds(own_tok, toks), pl.ds(mate_tok, toks)
        swaps, scatters, lasts = [], [], []

        def own_block(u):
            return block_cols((p + ring + (2 * c - 1) * u) % ring, c)

        def stage_swap(u):
            columns = block_cols((p + ring + (1 - 2 * c) * u) % ring, 1 - c)
            dsend[l, u] = jnp.dot(act[...], wo[l, :, columns], preferred_element_type=F32).astype(BF16)
            swaps.append(message(slot + u, dsend.at[l, u], drecv.at[l, u], d_dev))

        def stage_scatter(u):
            weights = wo[l, :, own_block(u)]
            away = jnp.dot(act[mate_rows, :], weights, preferred_element_type=F32)
            mine = jnp.dot(act[own_rows, :], weights, preferred_element_type=F32)
            swaps[u].wait()
            xsend[l, u] = (away + drecv[l, u, mate_rows, :].astype(F32)).astype(BF16)
            scatters.append(message(slot + ring + u, xsend.at[l, u], xrecv.at[l, u], x_dev))
            keep[u] = (mine + drecv[l, u, own_rows, :].astype(F32)
                       + source[:, own_block(u)].astype(F32))

        def stage_last(u):
            scatters[u].wait()
            strm[l, :, own_block(u)] = (keep[u] + xrecv[l, u].astype(F32)).astype(BF16)
            piece = strm.at[l, :, own_block(u)]
            lasts.append(message(slot + 2 * ring + u, piece, piece, d_dev))

        lag = 2
        for u in range(ring + 1 + lag):
            if u < ring:
                ensure(l, 1, u)
                stage_swap(u)
            if 1 <= u <= ring:
                stage_scatter(u - 1)
            if u % 3 == 1:
                pumps(1 if l + 1 < layers else 0)
            if u >= 1 + lag:
                stage_last(u - 1 - lag)
        for m in lasts:
            m.wait()

    out[...] = strm[layers - 1]


def fused(n, layers):
    def body(stream_in, norm_gain, value_weight, gate_weight, conv_taps, channel_gain, out_weight):
        toks, width = stream_in.shape
        taps_n = conv_taps.shape[1]
        rows, cols = value_weight.shape[1], value_weight.shape[2]
        ch, half, group, ring = cols // 2, width // 2, 2 * toks, n // 2
        i = lax.axis_index("sp") % 2
        taps = lax.dynamic_slice_in_dim(conv_taps, i * ch, ch, axis=2)
        vmem = pl.BlockSpec(memory_space=pltpu.VMEM)
        hbm = pl.BlockSpec(memory_space=pltpu.HBM)
        msgs = layers * (6 + ring * 3)
        return pl.pallas_call(
            functools.partial(kernel, n, layers, taps_n),
            out_shape=jax.ShapeDtypeStruct((toks, width), BF16),
            in_specs=[vmem, vmem, hbm, hbm, vmem, vmem, hbm],
            out_specs=vmem,
            scratch_shapes=[
                pltpu.VMEM((layers, width, ch), BF16),
                pltpu.VMEM((layers, width, ch), BF16),
                pltpu.VMEM((layers, ch, width), BF16),
                pltpu.VMEM((layers, group, width), BF16),
                pltpu.VMEM((PAD + group, ch), F32),
                pltpu.VMEM((layers, PAD, ch), BF16),
                pltpu.VMEM((layers, PAD, ch), BF16),
                pltpu.VMEM((group, ch), F32),
                pltpu.VMEM((layers, 8, group), F32),
                pltpu.VMEM((layers, 3, 8, group), F32),
                pltpu.VMEM((group, ch), BF16),
                pltpu.VMEM((layers, ring, group, rows), BF16),
                pltpu.VMEM((layers, ring, group, rows), BF16),
                pltpu.VMEM((layers, ring, toks, rows), BF16),
                pltpu.VMEM((layers, ring, toks, rows), BF16),
                pltpu.VMEM((layers, toks, width), BF16),
                pltpu.VMEM((ring, toks, rows), F32),
                pltpu.SemaphoreType.DMA((layers * 3,)),
                pltpu.SemaphoreType.DMA((layers * 3,)),
                pltpu.SemaphoreType.DMA((layers * 3,)),
                pltpu.SemaphoreType.DMA((layers * 4, 2 * SPLIT)),
                pltpu.SemaphoreType.DMA((layers * 4, 2 * SPLIT, ring - 1)),
                pltpu.SemaphoreType.DMA((msgs,)),
                pltpu.SemaphoreType.DMA((msgs,)),
            ],
            compiler_params=pltpu.CompilerParams(
                collective_id=0, has_side_effects=True, vmem_limit_bytes=62 * 2**20),
        )(stream_in, norm_gain, value_weight, gate_weight, taps, channel_gain, out_weight)

    return body


def passed_along(value, axis, steps):
    count = lax.axis_size(axis)
    leading, last = (max(0, -steps), min(count, count - steps))
    return lax.ppermute(value, axis, [(source, source + steps) for source in range(leading, last)])


def general(stream_in, norm_gain, value_weight, gate_weight, conv_taps, channel_gain, out_weight):
    stream = stream_in
    tok_rows = stream_in.shape[0]
    width = stream_in.shape[1]
    taps_n = conv_taps.shape[1]
    local_cols = value_weight.shape[2]
    for layer in range(norm_gain.shape[0]):
        wide = stream.astype(F32)
        normed = (
            wide
            * lax.rsqrt(jnp.mean(wide * wide, axis=1, keepdims=True) + epsilon)
            * norm_gain[layer]
        ).astype(BF16)
        value = jnp.dot(normed, lax.all_gather(value_weight[layer], "sp", axis=0, tiled=True),
                        preferred_element_type=F32)
        gate = jnp.dot(normed, lax.all_gather(gate_weight[layer], "sp", axis=0, tiled=True),
                       preferred_element_type=F32)
        gated = (value * jax.nn.sigmoid(gate)).astype(BF16)
        earlier = passed_along(gated[tok_rows - (taps_n - 1):], "sp", 1)
        padded = jnp.concatenate([earlier, gated], axis=0).astype(F32)
        taps = conv_taps[layer]
        filtered = jnp.zeros((tok_rows, local_cols), F32)
        for tap in range(taps_n):
            filtered = filtered + taps[tap] * padded[tap:tap + tok_rows]
        sum_first, sum_second = lax.psum(
            (jnp.sum(filtered, axis=1), jnp.sum(filtered * filtered, axis=1)), "tp")
        mean_value = (sum_first / width)[:, None]
        variance = (sum_second / width)[:, None] - mean_value * mean_value
        activated = jax.nn.silu(
            (filtered - mean_value) * lax.rsqrt(variance + epsilon) * channel_gain[layer]
        ).astype(BF16)
        whole_out = lax.all_gather(out_weight[layer], "sp", axis=1, tiled=True)
        terms = jnp.dot(activated, whole_out, preferred_element_type=F32)
        summed = lax.psum(terms.astype(BF16), "tp").astype(F32)
        stream = (wide + summed).astype(BF16)
    return stream


def solution(mesh):
    n, tp = mesh.shape["sp"], mesh.shape["tp"]

    def body(stream_in, norm_gain, value_weight, *rest):
        rows, cols = value_weight.shape[1], value_weight.shape[2]
        pairs = tp == 2 and n % 4 == 0 and rows % 128 == 0 and cols % 1024 == 0
        fits = stream_in.shape[0] % 64 == 0 and rest[1].shape[1] <= PAD
        chosen = fused(n, norm_gain.shape[0]) if pairs and fits else general
        return chosen(stream_in, norm_gain, value_weight, *rest)

    return jax.shard_map(
        body,
        mesh=mesh,
        in_specs=(
            P("sp", None),
            P(),
            P(None, "sp", "tp"),
            P(None, "sp", "tp"),
            P(None, None, "tp"),
            P(None, "tp"),
            P(None, "tp", "sp"),
        ),
        out_specs=P("sp", None),
        check_vma=False,
    )
```

```python
import functools

import jax
import jax.numpy as jnp
from jax import lax
from jax.experimental import pallas as pl
from jax.experimental.pallas import tpu as pltpu
from jax.sharding import PartitionSpec as P

epsilon = 1e-05
MESH = pl.DeviceIdType.MESH
F32 = jnp.float32
BF16 = jnp.bfloat16
PAD = 32
EARLY, EARLY_LAST = 3, 2
SPLIT = 1


def kernel(n, layers, taps_n, stream_in, gain, vw, gw, taps, cgain, ow, out,
           wv, wg, wo, nrm, gat, hsend, hrecv, fil, ssend, srecv, act,
           dsend, drecv, xsend, xrecv, strm, keep,
           loc_sem, wx_send, wx_recv, ring_send, ring_recv, msg_send, msg_recv):
    ring = n // 2
    s = lax.axis_index("sp")
    c = lax.axis_index("tp")
    o, i = s // 2, s % 2
    toks, width = stream_in.shape
    group = 2 * toks
    rows, cols = vw.shape[1], vw.shape[2]
    ch = cols // 2
    half = width // 2

    def place(outer):
        z, y = outer // 2, outer % 2
        return (1 - y) * z + y * (ring - 1 - z)

    def outer_at(pos):
        h = pos // (ring // 2)
        return 2 * ((1 - h) * pos + h * (ring - 1 - pos)) + h

    p = place(o)
    nxt = outer_at((p + 1) % ring) * 2 + i
    prv = outer_at((p + ring - 1) % ring) * 2 + i
    mate = o * 2 + 1 - i
    up = ((o + 1) % ring) * 2 + i
    down = ((o + ring - 1) % ring) * 2 + i
    x_dev, d_dev, xd_dev = (mate, c), (s, 1 - c), (mate, 1 - c)

    barrier = pltpu.get_barrier_semaphore()
    everyone = [x_dev, d_dev, xd_dev, (nxt, c), (prv, c), (up, c), (down, c)]
    for dev in everyone:
        pl.semaphore_signal(barrier, inc=1, device_id=dev, device_id_type=MESH)
    pl.semaphore_wait(barrier, len(everyone))

    def al(v, m):
        return pl.multiple_of(v, m)

    my_rows = pl.ds(al(s * rows, rows), rows)
    my_cols = pl.ds(al(i * ch, ch), ch)
    mate_cols = pl.ds(al((1 - i) * ch, ch), ch)

    def weight_views(l, kind):
        if kind == 0:
            return vw.at[l, :, my_cols], vw.at[l, :, mate_cols], wv.at[l, my_rows, :]
        if kind == 1:
            return gw.at[l, :, my_cols], gw.at[l, :, mate_cols], wg.at[l, my_rows, :]
        return ow.at[l, my_cols, :], ow.at[l, mate_cols, :], wo.at[l, :, my_rows]

    local, crossed = {}, {}

    def start_local(l, kind):
        src, _, dst = weight_views(l, kind)
        local[l, kind] = pltpu.make_async_copy(src, dst, loc_sem.at[l * 3 + kind])
        local[l, kind].start()

    def start_cross(l, kind):
        _, src, dst = weight_views(l, kind)
        crossed[l, kind] = pltpu.make_async_remote_copy(
            src, dst, wx_send.at[l * 3 + kind], wx_recv.at[l * 3 + kind],
            device_id=x_dev, device_id_type=MESH)
        crossed[l, kind].start()

    pending = {}

    def block_cols(pos, d):
        return pl.ds(al((outer_at(pos) * 2 + d) * rows, rows), rows)

    def chunk(l, grp, d, q, pos):
        if grp == 0:
            block = outer_at(pos) * 2 + (i + q // SPLIT) % 2
            w, size = (wv if d == 0 else wg), rows // SPLIT
            return w.at[l, pl.ds(al(block * rows + q % SPLIT * size, size), size), :]
        size = ch // 2 // SPLIT
        return wo.at[l, pl.ds(q * size, size), block_cols(pos, d)]

    def own_ready(l, grp, q):
        if grp == 0 and q % SPLIT == 0:
            for kind in (0, 1):
                (crossed if q else local)[l, kind].wait()
        if grp == 1 and q == 0:
            local[l, 2].wait()
            crossed[l, 2].wait()

    def pump(l, grp, t):
        for q in range(2 * SPLIT):
            if t == 0:
                own_ready(l, grp, q)
            for d in range(2):
                k = (l * 2 + grp) * 2 + d
                if t > 0:
                    pending[k, q].wait()
                if t < ring - 1:
                    pos = (p + ring - t) % ring if d == 0 else (p + t) % ring
                    ref = chunk(l, grp, d, q, pos)
                    pending[k, q] = pltpu.make_async_remote_copy(
                        ref, ref, ring_send.at[k, q], ring_recv.at[k, q, t],
                        device_id=(nxt if d == 0 else prv, c), device_id_type=MESH)
                    pending[k, q].start()

    queue = []
    for l in range(layers):
        main = [(l, 0, t) for t in range(1 if l else 0, ring)]
        side = [(l, 1, t) for t in range(ring)]
        early = min(EARLY if l + 1 < layers else EARLY_LAST, ring)
        queue += main[:len(main) - early]
        for t in range(early):
            queue += [main[len(main) - early + t], side[t]]
        rest = side[early:]
        queue += rest[:len(rest) // 2]
        if l + 1 < layers:
            queue.append((l + 1, 0, 0))
        queue += rest[len(rest) // 2:]
    done = []

    def pumps(count):
        for _ in range(count):
            if queue:
                item = queue.pop(0)
                pump(*item)
                done.append(item)

    def ensure(l, grp, t):
        while (l, grp, t) not in done:
            pumps(1)

    def message(slot, src, dst, dev):
        m = pltpu.make_async_remote_copy(src, dst, msg_send.at[slot], msg_recv.at[slot],
                                         device_id=dev, device_id_type=MESH)
        m.start()
        return m

    for l in range(layers):
        for kind in range(3):
            start_local(l, kind)
    start_cross(0, 0)
    start_cross(0, 1)

    own_tok = al(i * toks, toks)
    mate_tok = al((1 - i) * toks, toks)
    own_half = pl.ds(al(c * half, half), half)
    tile = 128 if toks % 128 == 0 else toks
    per_layer = 6 + ring * 3

    for l in range(layers):
        base = l * per_layer
        source = stream_in if l == 0 else strm.at[l - 1]

        def norm_step(r, _):
            at = al(r * 64, 64)
            wide = source[pl.ds(at, 64), :].astype(F32)
            scale = lax.rsqrt(jnp.mean(wide * wide, axis=1, keepdims=True) + epsilon)
            nrm[l, pl.ds(al(own_tok + at, 64), 64), :] = (wide * scale * gain[l:l + 1, :]).astype(BF16)
            return 0

        lax.fori_loop(0, toks // 64, norm_step, 0)
        spot = nrm.at[l, pl.ds(own_tok, toks), own_half]
        got = nrm.at[l, pl.ds(mate_tok, toks), own_half]
        gather = message(base + 0, spot, spot, x_dev)
        if l == 0:
            start_cross(0, 2)
            for ll in range(1, layers):
                for kind in range(3):
                    start_cross(ll, kind)
            pumps(3)
        else:
            pumps(4)
        gather.wait()
        relay = message(base + 1, got, got, d_dev)
        ensure(l, 0, ring - 1)
        relay.wait()

        def gate_step(r, _):
            at = al(r * tile, tile)
            x = nrm[l, pl.ds(at, tile), :]
            value = jnp.dot(x, wv[l], preferred_element_type=F32)
            gate = jnp.dot(x, wg[l], preferred_element_type=F32)
            gated = (value * jax.nn.sigmoid(gate)).astype(BF16)
            gat[pl.ds(al(PAD + at, 32), tile), :] = gated.astype(F32)
            return 0

        lax.fori_loop(0, group // tile, gate_step, 0)
        hsend[l] = gat[group:group + PAD, :].astype(BF16)
        halo = message(base + 2, hsend.at[l], hrecv.at[l], (up, c))
        pumps(1)
        halo.wait()
        first = (o > 0).astype(F32)
        gat[0:PAD, :] = hrecv[l].astype(F32) * first

        lead = PAD - (taps_n - 1)
        step_rows = 64
        lanes = 128

        def conv_step(r, _):
            at = al(r * step_rows, step_rows)
            for lane in range(ch // lanes):
                cut = slice(lane * lanes, (lane + 1) * lanes)
                total = jnp.zeros((step_rows, lanes), F32)
                block = gat[pl.ds(at, step_rows + PAD), cut]
                for b in range(8):
                    moved = block if b == 0 else pltpu.roll(block, step_rows + PAD - b, 0)
                    for a in range(PAD // 8 + 1):
                        tap = 8 * a + b - lead
                        if 0 <= tap < taps_n:
                            total = total + taps[l, tap:tap + 1, cut] * moved[8 * a:8 * a + step_rows]
                fil[pl.ds(at, step_rows), cut] = total
            return 0

        parts = 2
        per = group // step_rows // parts
        for part in range(parts):
            lax.fori_loop(part * per, (part + 1) * per, conv_step, 0)
            pumps(1)

        wide = fil[...]
        first_sum = jnp.sum(wide, axis=1, keepdims=True)
        second_sum = jnp.sum(wide * wide, axis=1, keepdims=True)
        lane_id = lax.broadcasted_iota(jnp.int32, (group, lanes), 1)
        stat = jnp.where(lane_id == 0, first_sum, jnp.where(lane_id == 1, second_sum, 0.0))
        ssend[l] = jnp.transpose(stat)[0:8, :]
        sums = [message(base + 3 + k, ssend.at[l], srecv.at[l, k], dev)
                for k, dev in enumerate((x_dev, d_dev, xd_dev))]
        pumps(1)
        for m in sums:
            m.wait()
        whole = ssend[l] + srecv[l, 0] + srecv[l, 1] + srecv[l, 2]
        stat = jnp.transpose(jnp.concatenate([whole] + [jnp.zeros((lanes - 8, group), F32)], axis=0))
        mean_value = stat[:, 0:1] / width
        variance = stat[:, 1:2] / width - mean_value * mean_value
        act[...] = jax.nn.silu((fil[...] - mean_value) * lax.rsqrt(variance + epsilon)
                               * cgain[l:l + 1, pl.ds(al(i * ch, ch), ch)]).astype(BF16)

        slot = base + 6
        own_rows, mate_rows = pl.ds(own_tok, toks), pl.ds(mate_tok, toks)
        swaps, scatters, lasts = [], [], []

        def own_block(u):
            return block_cols((p + ring + (2 * c - 1) * u) % ring, c)

        def stage_swap(u):
            columns = block_cols((p + ring + (1 - 2 * c) * u) % ring, 1 - c)
            dsend[l, u] = jnp.dot(act[...], wo[l, :, columns], preferred_element_type=F32).astype(BF16)
            swaps.append(message(slot + u, dsend.at[l, u], drecv.at[l, u], d_dev))

        def stage_scatter(u):
            weights = wo[l, :, own_block(u)]
            away = jnp.dot(act[mate_rows, :], weights, preferred_element_type=F32)
            mine = jnp.dot(act[own_rows, :], weights, preferred_element_type=F32)
            swaps[u].wait()
            xsend[l, u] = (away + drecv[l, u, mate_rows, :].astype(F32)).astype(BF16)
            scatters.append(message(slot + ring + u, xsend.at[l, u], xrecv.at[l, u], x_dev))
            keep[u] = (mine + drecv[l, u, own_rows, :].astype(F32)
                       + source[:, own_block(u)].astype(F32))

        def stage_last(u):
            scatters[u].wait()
            strm[l, :, own_block(u)] = (keep[u] + xrecv[l, u].astype(F32)).astype(BF16)
            piece = strm.at[l, :, own_block(u)]
            lasts.append(message(slot + 2 * ring + u, piece, piece, d_dev))

        lag = 2
        for u in range(ring + 1 + lag):
            if u < ring:
                ensure(l, 1, u)
                stage_swap(u)
            if 1 <= u <= ring:
                stage_scatter(u - 1)
            if u % 3 == 1:
                pumps(1 if l + 1 < layers else 0)
            if u >= 1 + lag:
                stage_last(u - 1 - lag)
        for m in lasts:
            m.wait()

    out[...] = strm[layers - 1]


def fused(n, layers):
    def body(stream_in, norm_gain, value_weight, gate_weight, conv_taps, channel_gain, out_weight):
        toks, width = stream_in.shape
        taps_n = conv_taps.shape[1]
        rows, cols = value_weight.shape[1], value_weight.shape[2]
        ch, half, group, ring = cols // 2, width // 2, 2 * toks, n // 2
        i = lax.axis_index("sp") % 2
        taps = lax.dynamic_slice_in_dim(conv_taps, i * ch, ch, axis=2)
        vmem = pl.BlockSpec(memory_space=pltpu.VMEM)
        hbm = pl.BlockSpec(memory_space=pltpu.HBM)
        msgs = layers * (6 + ring * 3)
        return pl.pallas_call(
            functools.partial(kernel, n, layers, taps_n),
            out_shape=jax.ShapeDtypeStruct((toks, width), BF16),
            in_specs=[vmem, vmem, hbm, hbm, vmem, vmem, hbm],
            out_specs=vmem,
            scratch_shapes=[
                pltpu.VMEM((layers, width, ch), BF16),
                pltpu.VMEM((layers, width, ch), BF16),
                pltpu.VMEM((layers, ch, width), BF16),
                pltpu.VMEM((layers, group, width), BF16),
                pltpu.VMEM((PAD + group, ch), F32),
                pltpu.VMEM((layers, PAD, ch), BF16),
                pltpu.VMEM((layers, PAD, ch), BF16),
                pltpu.VMEM((group, ch), F32),
                pltpu.VMEM((layers, 8, group), F32),
                pltpu.VMEM((layers, 3, 8, group), F32),
                pltpu.VMEM((group, ch), BF16),
                pltpu.VMEM((layers, ring, group, rows), BF16),
                pltpu.VMEM((layers, ring, group, rows), BF16),
                pltpu.VMEM((layers, ring, toks, rows), BF16),
                pltpu.VMEM((layers, ring, toks, rows), BF16),
                pltpu.VMEM((layers, toks, width), BF16),
                pltpu.VMEM((ring, toks, rows), F32),
                pltpu.SemaphoreType.DMA((layers * 3,)),
                pltpu.SemaphoreType.DMA((layers * 3,)),
                pltpu.SemaphoreType.DMA((layers * 3,)),
                pltpu.SemaphoreType.DMA((layers * 4, 2 * SPLIT)),
                pltpu.SemaphoreType.DMA((layers * 4, 2 * SPLIT, ring - 1)),
                pltpu.SemaphoreType.DMA((msgs,)),
                pltpu.SemaphoreType.DMA((msgs,)),
            ],
            compiler_params=pltpu.CompilerParams(
                collective_id=0, has_side_effects=True, vmem_limit_bytes=62 * 2**20),
        )(stream_in, norm_gain, value_weight, gate_weight, taps, channel_gain, out_weight)

    return body


def passed_along(value, axis, steps):
    count = lax.axis_size(axis)
    leading, last = (max(0, -steps), min(count, count - steps))
    return lax.ppermute(value, axis, [(source, source + steps) for source in range(leading, last)])


def general(stream_in, norm_gain, value_weight, gate_weight, conv_taps, channel_gain, out_weight):
    stream = stream_in
    tok_rows = stream_in.shape[0]
    width = stream_in.shape[1]
    taps_n = conv_taps.shape[1]
    local_cols = value_weight.shape[2]
    for layer in range(norm_gain.shape[0]):
        wide = stream.astype(F32)
        normed = (
            wide
            * lax.rsqrt(jnp.mean(wide * wide, axis=1, keepdims=True) + epsilon)
            * norm_gain[layer]
        ).astype(BF16)
        value = jnp.dot(normed, lax.all_gather(value_weight[layer], "sp", axis=0, tiled=True),
                        preferred_element_type=F32)
        gate = jnp.dot(normed, lax.all_gather(gate_weight[layer], "sp", axis=0, tiled=True),
                       preferred_element_type=F32)
        gated = (value * jax.nn.sigmoid(gate)).astype(BF16)
        earlier = passed_along(gated[tok_rows - (taps_n - 1):], "sp", 1)
        padded = jnp.concatenate([earlier, gated], axis=0).astype(F32)
        taps = conv_taps[layer]
        filtered = jnp.zeros((tok_rows, local_cols), F32)
        for tap in range(taps_n):
            filtered = filtered + taps[tap] * padded[tap:tap + tok_rows]
        sum_first, sum_second = lax.psum(
            (jnp.sum(filtered, axis=1), jnp.sum(filtered * filtered, axis=1)), "tp")
        mean_value = (sum_first / width)[:, None]
        variance = (sum_second / width)[:, None] - mean_value * mean_value
        activated = jax.nn.silu(
            (filtered - mean_value) * lax.rsqrt(variance + epsilon) * channel_gain[layer]
        ).astype(BF16)
        whole_out = lax.all_gather(out_weight[layer], "sp", axis=1, tiled=True)
        terms = jnp.dot(activated, whole_out, preferred_element_type=F32)
        summed = lax.psum(terms.astype(BF16), "tp").astype(F32)
        stream = (wide + summed).astype(BF16)
    return stream


def solution(mesh):
    n, tp = mesh.shape["sp"], mesh.shape["tp"]

    def body(stream_in, norm_gain, value_weight, *rest):
        rows, cols = value_weight.shape[1], value_weight.shape[2]
        pairs = tp == 2 and n % 4 == 0 and rows % 128 == 0 and cols % 1024 == 0
        fits = stream_in.shape[0] % 64 == 0 and rest[1].shape[1] <= PAD
        chosen = fused(n, norm_gain.shape[0]) if pairs and fits else general
        return chosen(stream_in, norm_gain, value_weight, *rest)

    return jax.shard_map(
        body,
        mesh=mesh,
        in_specs=(
            P("sp", None),
            P(),
            P(None, "sp", "tp"),
            P(None, "sp", "tp"),
            P(None, None, "tp"),
            P(None, "tp"),
            P(None, "tp", "sp"),
        ),
        out_specs=P("sp", None),
        check_vma=False,
    )
```
